512 devices in a mesh: grp: 2 (over y), kv: 32 (over z), tp: 8 (over x, core).
Axes of the slice: x: 4, y: 2, z: 32, core: 2. Of those that a mesh axis runs over, the one named last changes fastest.
The devices are a block of a 4x8x32 slice.
Arguments:
- tokens: bfloat16 [256, 4096], P('grp', 'kv'), parts along dimension 0, may hold values from -100 to 100
- norm_gain: bfloat16 [4096], P('kv'), may hold values from 0.099609375 to 1.8984375
- w_query1: bfloat16 [4096, 1024], P('kv', 'tp'), may hold values from -0.15625 to 0.15625
- w_query2: bfloat16 [4096, 1024], P('kv', 'tp'), may hold values from -0.15625 to 0.15625
- w_key1: bfloat16 [4096, 1024], P('kv', 'tp'), may hold values from -0.09375 to 0.09375
- w_key2: bfloat16 [4096, 1024], P('kv', 'tp'), may hold values from -0.09375 to 0.09375
- w_value: bfloat16 [4096, 2048], P('kv', 'tp'), may hold values from -0.09375 to 0.09375
- head_gain: bfloat16 [128], replicated, may hold values from 0.099609375 to 1.8984375
- lambdas: float32 [16], P('tp'), may hold values from 0.3 to 0.8
- w_out: bfloat16 [2048, 4096], P('tp', 'kv'), may hold values from -0.125 to 0.125
- cache_keys: bfloat16 [16, 8192, 16, 128], P('grp', 'kv', 'tp'), parts along dimension 0, may hold values from -330 to 330
- cache_values: bfloat16 [16, 8192, 16, 128], P('grp', 'kv', 'tp'), parts along dimension 0, may hold values from -6 to 6
- lengths: int32 [16], P('grp'), parts along dimension 0, may hold values from 4096 to 8160
- accepted: int32 [16], P('grp'), parts along dimension 0, may hold values from 0 to 16
- parents: int32 [16, 16], P('grp'), parts along dimension 0, may hold values from -1 to 14, as said below
Outputs:
- mixed: bfloat16 [256, 4096], P(('grp', 'tp'), 'kv'), parts along dimension 0
- new_keys: bfloat16 [16, 8192, 16, 128], P('grp', 'kv', 'tp'), parts along dimension 0
- new_values: bfloat16 [16, 8192, 16, 128], P('grp', 'kv', 'tp'), parts along dimension 0
The draws below stay inside these ranges and needn't reach their ends.
There are 2 independent parts, one for each index of `grp`. The reference program is written for one: setup_inputs(seed, part) draws one part's arguments, and reference() takes and returns one part's arrays. A program takes and returns all parts, laid end to end along the dimension named above; an argument that names none is the same for every part. Nothing has to cross between parts.
Inputs may be any that keep to these rules, and one draw needn't show every extreme that they name: parents[s, 0] = -1; for j of 1 onward parents[s, j] lies between 0 and j - 1.
All inputs are finite; a program needn't handle non-finite values.
Results may differ from the reference program's by a relative error of at most 0.01225.
The reference program's roundings to bfloat16 on the way count: a program that leaves them out, or rounds other values in their place, can miss the bound.
Values may be sent and summed in bfloat16 or wider, within the bound.
No kernel may reach another device: no remote copies, remote signals or barrier semaphores. Data moves between devices by JAX's collectives and lax.ppermute only.
A program may use at most 64 MiB of HBM per device.

```python
import jax
import jax.numpy as jnp
from jax import lax

D = 4096
HEADS = 16
QK_DIM = 64
V_DIM = 128
PROP = 16
SEQS = 8
CTX_DEV = 256
CTX = 8192
TOKENS = 128
N_KV = 32
N_TP = 8


def draw_tokens(key, part):
    key_one = jax.random.fold_in(jax.random.fold_in(key, 11), 0)
    columns = jnp.exp(jnp.log(5.0) * jnp.arange(D, dtype=jnp.float32) / D)
    sample = jax.random.truncated_normal(key_one, -5.0, 5.0, (TOKENS, D), jnp.float32)
    return (sample * columns[None, :]).astype(jnp.bfloat16)


def draw_cache_keys(key, part):
    key_one = jax.random.fold_in(jax.random.fold_in(key, 23), 0)
    array_shape = (SEQS, CTX, HEADS, 2 * QK_DIM)
    sample = jax.random.truncated_normal(key_one, -4.0, 4.0, array_shape, jnp.float32)
    return sample.astype(jnp.bfloat16)


def draw_parents(key, part):
    nodes = jnp.arange(PROP, dtype=jnp.int32)
    chosen = jax.random.randint(jax.random.fold_in(key, 37), (SEQS, PROP), 0, jnp.maximum(nodes, 1)[None, :])
    return jnp.where(nodes[None, :] == 0, -1, chosen).astype(jnp.int32)


def plant(array, own_key, least, high):
    dims = array.shape
    spot = [jax.random.randint(jax.random.fold_in(own_key, axis), (), 0, dims[axis]) for axis in range(len(dims))]
    array = array.at[tuple(spot)].set(least)
    longest = dims.index(max(dims))
    spot[longest] = (spot[longest] + 1) % dims[longest]
    return array.at[tuple(spot)].set(high)


def block_scale(stream_key, dims, pieces, least, high):
    def one(axis_at, blocks):
        steps = jax.random.uniform(jax.random.fold_in(jax.random.fold_in(stream_key, 6), axis_at), (blocks,), jnp.float32, least / len(pieces), high / len(pieces))
        return jnp.repeat(jnp.exp(steps), dims[axis_at] // blocks).reshape((-1,) + (1,) * (len(dims) - axis_at - 1))

    level = one(*pieces[0])
    for cut in pieces[1:]:
        level = level * one(*cut)
    return level


def noise(key, shape, scale, most, cuts=(), kind=jnp.bfloat16):
    array = scale * jax.random.normal(key, shape, jnp.float32)
    if cuts:
        array = array * block_scale(key, shape, cuts, -0.22, 0.18)
    return jnp.clip(array, -most, most).astype(kind)


def setup_inputs(seed: int = 0, part: int = 0) -> dict:
    key_list = jax.random.split(jax.random.key(seed), 16)
    own_keys = jax.random.split(jax.random.fold_in(key_list[15], part), 16)
    tokens = draw_tokens(jax.random.fold_in(jax.random.fold_in(key_list[15], part), 71), part)
    norm_gain = jnp.clip(1.0 + 0.18 * jax.random.normal(key_list[1], (D,), jnp.float32), 0.099609375, 1.8984375).astype(jnp.bfloat16)
    w_query1 = noise(key_list[2], (D, HEADS * QK_DIM), (D // 3) ** -0.5, 0.15625, ((0, 32), (1, 8)))
    w_query2 = noise(key_list[3], (D, HEADS * QK_DIM), (D // 3) ** -0.5, 0.15625, ((0, 32), (1, 8)))
    w_key1 = noise(key_list[4], (D, HEADS * QK_DIM), D ** -0.5, 0.09375, ((0, 32), (1, 8)))
    w_key2 = noise(key_list[5], (D, HEADS * QK_DIM), D ** -0.5, 0.09375, ((0, 32), (1, 8)))
    w_value = noise(key_list[6], (D, HEADS * V_DIM), D ** -0.5, 0.09375, ((0, 32), (1, 8)))
    head_gain = jnp.clip(1.0 + 0.18 * jax.random.normal(key_list[7], (V_DIM,), jnp.float32), 0.099609375, 1.8984375).astype(jnp.bfloat16)
    lambdas = jnp.clip(0.3 + 0.5 * jax.random.uniform(key_list[8], (HEADS,), jnp.float32) ** block_scale(key_list[8], (HEADS,), ((0, 8),), -0.2, 0.2), 0.3, 0.8)
    w_out = noise(key_list[9], (HEADS * V_DIM, D), (HEADS * V_DIM) ** -0.5, 0.125, ((0, 8), (1, 32)))
    cache_keys = draw_cache_keys(jax.random.fold_in(jax.random.fold_in(key_list[15], part), 71), part)
    cache_values = noise(own_keys[11], (SEQS, CTX, HEADS, V_DIM), 1.0, 6.0, ((1, 32), (2, 8)))
    lengths = plant(jax.random.randint(own_keys[12], (SEQS,), CTX // 2, CTX - 2 * PROP + 1), jax.random.fold_in(own_keys[12], 1), CTX // 2, CTX - 2 * PROP).astype(jnp.int32)
    accepted = plant(jax.random.randint(own_keys[13], (SEQS,), 0, PROP + 1), jax.random.fold_in(own_keys[13], 1), 0, PROP).astype(jnp.int32)
    parents = draw_parents(jax.random.fold_in(jax.random.fold_in(key_list[15], part), 71), part)
    return {"tokens": tokens, "norm_gain": norm_gain, "w_query1": w_query1, "w_query2": w_query2, "w_key1": w_key1, "w_key2": w_key2, "w_value": w_value, "head_gain": head_gain, "lambdas": lambdas, "w_out": w_out, "cache_keys": cache_keys, "cache_values": cache_values, "lengths": lengths, "accepted": accepted, "parents": parents}


epsilon = 1e-06
masked_fill = -1e+30
head_factor = 0.8

def ancestor_mask(parents, width):
    nodes = jnp.arange(width, dtype=jnp.int32)
    closure = (parents[:, :, None] == nodes[None, None, :]).astype(jnp.float32)
    closure = closure + jnp.eye(width, dtype=jnp.float32)[None]
    for repeat in range(width.bit_length()):
        closure = jnp.minimum(jnp.einsum('sji,sik->sjk', closure, closure, precision=lax.Precision.HIGHEST), 1.0)
    return closure > 0.5

def rounded(values):
    return lax.optimization_barrier(values.astype(jnp.bfloat16)).astype(jnp.float32)

def place(cache_rows, fresh_rows, start_pos):
    anchor = jnp.zeros((), jnp.int32)
    return lax.dynamic_update_slice(cache_rows, fresh_rows, (start_pos.astype(jnp.int32), anchor, anchor))

def reference(tokens, norm_gain, w_query1, w_query2, w_key1, w_key2, w_value, head_gain, lambdas, w_out, cache_keys, cache_values, lengths, accepted, parents):
    wide_tokens = tokens.astype(jnp.float32)
    inverse_rms = lax.rsqrt(lax.optimization_barrier(jnp.mean(wide_tokens * wide_tokens, axis=1)) + epsilon)
    scaled = (wide_tokens * norm_gain.astype(jnp.float32)[None, :]).astype(jnp.bfloat16)

    def project(weight, factor, width):
        product = jnp.dot(scaled, weight, preferred_element_type=jnp.float32)
        return (product * inverse_rms[:, None] * factor).astype(jnp.bfloat16).reshape(SEQS, PROP, HEADS, width)
    query_one = project(w_query1, QK_DIM ** (-0.5), QK_DIM)
    query_two = project(w_query2, QK_DIM ** (-0.5), QK_DIM)
    key_one = project(w_key1, 1.0, QK_DIM)
    key_two = project(w_key2, 1.0, QK_DIM)
    value_new = project(w_value, 1.0, V_DIM)
    key_new = jnp.concatenate([key_one, key_two], axis=-1)
    valid_len = lengths + accepted
    tree_mask = ancestor_mask(parents, PROP)

    def one_sequence(members):
        first_query, second_query, fresh_keys, fresh_values, old_keys, old_values, limit_one, tree_seen = members
        places = jnp.arange(CTX, dtype=jnp.int32).reshape(N_KV, CTX_DEV)
        visible = (places < limit_one)[:, None, None, :]
        blocked_keys = old_keys.reshape(N_KV, CTX_DEV, HEADS, 2 * QK_DIM).astype(jnp.float32)
        blocked_values = old_values.reshape(N_KV, CTX_DEV, HEADS, V_DIM).astype(jnp.float32)
        tree_keys = fresh_keys.astype(jnp.float32)
        tree_values = fresh_values.astype(jnp.float32)
        tree_visible = tree_seen[:, None, :]

        def attend(queries, cache_part, tree_part):
            wide_query = queries.astype(jnp.float32)
            cache_scores = jnp.einsum('jhd,bchd->bjhc', wide_query, cache_part)
            cache_scores = jnp.where(visible, cache_scores, masked_fill)
            cache_max = lax.optimization_barrier(jnp.max(cache_scores, axis=-1))
            cache_exp = jnp.where(visible, jnp.exp(cache_scores - cache_max[..., None]), 0.0)
            cache_total = lax.optimization_barrier(jnp.sum(cache_exp, axis=-1))
            cache_out = jnp.einsum('bjhc,bche->bjhe', rounded(cache_exp), blocked_values)
            tree_scores = jnp.einsum('jhd,ihd->jhi', wide_query, tree_part)
            tree_scores = jnp.where(tree_visible, tree_scores, masked_fill)
            tree_max = lax.optimization_barrier(jnp.max(tree_scores, axis=-1))
            tree_exp = jnp.where(tree_visible, jnp.exp(tree_scores - tree_max[..., None]), 0.0)
            tree_total = lax.optimization_barrier(jnp.sum(tree_exp, axis=-1))
            tree_out = jnp.einsum('jhi,ihe->jhe', rounded(tree_exp), tree_values)
            highest = jnp.maximum(lax.optimization_barrier(jnp.max(cache_max, axis=0)), tree_max)
            cache_scale = jnp.exp(cache_max - highest[None])
            tree_scale = jnp.exp(tree_max - highest)
            totals = lax.optimization_barrier(jnp.sum(cache_scale * cache_total, axis=0)) + tree_scale * tree_total
            summed = lax.optimization_barrier(jnp.sum(cache_scale[..., None] * cache_out, axis=0)) + tree_scale[..., None] * tree_out
            return summed / totals[..., None]
        attention_one = attend(first_query, blocked_keys[..., :QK_DIM], tree_keys[..., :QK_DIM])
        attention_two = attend(second_query, blocked_keys[..., QK_DIM:], tree_keys[..., QK_DIM:])
        differ = attention_one - lambdas[None, :, None] * attention_two
        normed = differ * lax.rsqrt(lax.optimization_barrier(jnp.mean(differ * differ, axis=-1, keepdims=True)) + epsilon)
        normed = normed * head_gain.astype(jnp.float32) * head_factor
        return normed.astype(jnp.bfloat16)
    head_out = lax.map(one_sequence, (query_one, query_two, key_new, value_new, cache_keys, cache_values, valid_len, tree_mask))
    head_out = head_out.reshape(TOKENS, HEADS * V_DIM)
    grouped = head_out.reshape(TOKENS, N_TP, HEADS * V_DIM // N_TP).astype(jnp.float32)
    weight_groups = w_out.reshape(N_TP, HEADS * V_DIM // N_TP, D).astype(jnp.float32)
    products = jnp.einsum('tgk,gkd->gtd', grouped, weight_groups)
    mixed = lax.optimization_barrier(jnp.sum(rounded(products), axis=0)).astype(jnp.bfloat16)
    new_keys = jax.vmap(place)(cache_keys, key_new, valid_len)
    new_values = jax.vmap(place)(cache_values, value_new, valid_len)
    return (mixed, new_keys, new_values)
```

```python
import functools

import jax
import jax.numpy as jnp
from jax import lax
from jax.experimental import pallas as pl
from jax.experimental.pallas import tpu as pltpu
from jax.sharding import PartitionSpec as P

epsilon = 1e-06
masked_fill = -1e30
head_factor = 0.8
LANES = 128
ROWS = 8

f32 = jnp.float32
bf16 = jnp.bfloat16
VMEM = pl.BlockSpec(memory_space=pltpu.VMEM)
SMEM = pl.BlockSpec(memory_space=pltpu.SMEM)


def call(body, out_shape, in_specs, name, flops, out_specs=VMEM, scratch=()):
    return pl.pallas_call(
        body,
        out_shape=out_shape,
        in_specs=in_specs,
        out_specs=out_specs,
        scratch_shapes=scratch,
        cost_estimate=pl.CostEstimate(flops=flops, bytes_accessed=1 << 16, transcendentals=0),
        name=name,
    )


def shape(dims, dtype):
    return jax.ShapeDtypeStruct(dims, dtype)


def lane_iota(dims):
    return lax.broadcasted_iota(jnp.int32, dims, len(dims) - 1)


def row_iota(dims):
    return lax.broadcasted_iota(jnp.int32, dims, len(dims) - 2)


def scale_tokens(tokens_ref, gain_ref):
    wide = tokens_ref[...].astype(f32)
    return wide, (wide * gain_ref[...].astype(f32)).astype(bf16)


def by_head(first, second, head):
    half = LANES // 2
    left = first[:, head * half : (head + 1) * half]
    right = second[:, head * half : (head + 1) * half]
    return jnp.concatenate([left, right], axis=1)


def query_parts(heads, tokens_ref, gain_ref, w1_ref, w2_ref, out_ref):
    wide, scaled = scale_tokens(tokens_ref, gain_ref)
    first = jnp.dot(scaled, w1_ref[...], preferred_element_type=f32)
    second = jnp.dot(scaled, w2_ref[...], preferred_element_type=f32)
    squares = jnp.sum(jnp.transpose(wide * wide), axis=0, keepdims=True)
    for head in range(heads):
        columns = by_head(first, second, head)
        for group in range(wide.shape[0] // ROWS):
            owner = group * heads + head
            for row in range(ROWS):
                at = group * ROWS + row
                out_ref[owner, :, row * LANES : (row + 1) * LANES] = columns[at : at + 1, :]
            out_ref[owner, :, ROWS * LANES :] = squares


def value_parts(heads, tokens_ref, gain_ref, w1_ref, w2_ref, wv_ref, out_ref):
    _, scaled = scale_tokens(tokens_ref, gain_ref)
    first = jnp.dot(scaled, w1_ref[...], preferred_element_type=f32)
    second = jnp.dot(scaled, w2_ref[...], preferred_element_type=f32)
    value = jnp.dot(scaled, wv_ref[...], preferred_element_type=f32)
    for head in range(heads):
        columns = by_head(first, second, head)
        for group in range(scaled.shape[0] // ROWS):
            rows = slice(group * ROWS, (group + 1) * ROWS)
            at = slice(head * LANES, (head + 1) * LANES)
            out_ref[group * heads, :, at] = columns[rows].astype(bf16)
            out_ref[group * heads + 1, :, at] = value[rows, at].astype(bf16)


def finish_queries(heads, width, factor, part_ref, out_ref, inverse_ref):
    group = lax.axis_index("kv") // heads
    total = part_ref[0]
    for source in range(1, part_ref.shape[0]):
        total = total + part_ref[source]
    inverse = lax.rsqrt(total[:, ROWS * LANES :] / width + epsilon)
    tile = (ROWS, LANES)
    mine = lane_iota(tile) == group * ROWS + row_iota(tile)
    column = jnp.sum(jnp.where(mine, inverse, 0.0), axis=1, keepdims=True)
    sums = jnp.concatenate(
        [total[:, row * LANES : (row + 1) * LANES] for row in range(ROWS)], axis=0
    )
    query = (sums * column * factor).astype(bf16)
    inverse_ref[...] = jnp.broadcast_to(column, tile)
    for owner in range(out_ref.shape[0]):
        out_ref[owner] = query


def finish_values(part_ref, inverse_ref, out_ref):
    total = part_ref[0].astype(f32)
    for source in range(1, part_ref.shape[0]):
        total = total + part_ref[source].astype(f32)
    column = inverse_ref[:, 0:1]
    fresh = (total * column).astype(bf16)
    for owner in range(out_ref.shape[0]):
        out_ref[owner] = fresh


def two_maps(query):
    low = lane_iota(query.shape) < LANES // 2
    zero = jnp.zeros_like(query)
    return jnp.concatenate(
        [jnp.where(low, query, zero), jnp.where(low, zero, query)], axis=0
    ).astype(bf16)


def softmax_block(scores, visible):
    scores = jnp.where(visible, scores, masked_fill)
    maxima = jnp.max(scores, axis=1, keepdims=True)
    weights = jnp.where(visible, jnp.exp(scores - maxima), 0.0)
    return maxima, jnp.sum(weights, axis=1, keepdims=True), weights.astype(bf16)


def contract_last(left, right):
    return lax.dot_general(left, right, (((1,), (1,)), ((), ())), preferred_element_type=f32)


def in_pieces(value):
    high = value.astype(bf16).astype(f32)
    rest = value - high
    middle = rest.astype(bf16).astype(f32)
    return (high, middle, rest - middle)


PIECES = 6


def attend_cache(heads, query_ref, keys_ref, values_ref, lengths_ref, accepted_ref, out_ref):
    seqs, context = keys_ref.shape[1], keys_ref.shape[2]
    start = lax.axis_index("kv") * context
    for seq in range(seqs):
        limit = lengths_ref[seq] + accepted_ref[seq] - start
        for head in range(heads):
            owners = [(2 * seq + half) * heads + head for half in range(2)]
            query = jnp.concatenate([query_ref[o].astype(f32) for o in owners], axis=0)
            both = two_maps(query)
            scores = contract_last(both, keys_ref[head, seq])
            visible = lane_iota(scores.shape) < limit
            maxima, totals, weights = softmax_block(scores, visible)
            summed = jnp.dot(weights, values_ref[head, seq], preferred_element_type=f32)
            dims = summed.shape
            count = dims[0] // 2
            at = lane_iota(dims) - jnp.where(row_iota(dims) >= count, PIECES, 0)
            stats = jnp.zeros(dims, f32)
            for k, piece in enumerate(in_pieces(maxima) + in_pieces(totals)):
                stats = jnp.where(at == k, piece, stats)
            for half, owner in enumerate(owners):
                low, high = half * ROWS, count + half * ROWS
                first, second = slice(low, low + ROWS), slice(high, high + ROWS)
                out_ref[owner, :, 0:LANES] = summed[first].astype(bf16)
                out_ref[owner, :, LANES : 2 * LANES] = summed[second].astype(bf16)
                out_ref[owner, :, 2 * LANES :] = (stats[first] + stats[second]).astype(bf16)


def attend_tree(heads, query_ref, fresh_ref, parents_ref, out_ref, seen_ref):
    me = lax.axis_index("kv")
    head, group = lax.rem(me, heads), me // heads
    seq, half = group // 2, lax.rem(group, 2)
    nodes = parents_ref.shape[1]
    for node in range(nodes):
        parent = parents_ref[seq, node]
        above = jnp.where(parent >= 0, seen_ref[jnp.maximum(parent, 0)], 0) if node else 0
        seen_ref[node] = above | (1 << node)

    def rows_of(kind):
        tiles = []
        for part in range(2):
            both = fresh_ref[(2 * seq + part) * heads + kind].astype(f32)
            tiles.append(jnp.where(head == 0, both[:, :LANES], both[:, LANES:]))
        tiles.append(jnp.zeros((LANES - nodes, LANES), f32))
        return jnp.concatenate(tiles, axis=0).astype(bf16)

    both = two_maps(query_ref[0].astype(f32))
    scores = contract_last(both, rows_of(0))
    dims = scores.shape
    row = lax.rem(row_iota(dims), ROWS)
    bits = jnp.zeros(dims, jnp.int32)
    for k in range(ROWS):
        bits = jnp.where(row == k, seen_ref[half * ROWS + k], bits)
    lane = lane_iota(dims)
    visible = (lane < nodes) & ((lax.shift_right_logical(bits, jnp.minimum(lane, 31)) & 1) == 1)
    maxima, totals, weights = softmax_block(scores, visible)
    out_ref[0] = jnp.broadcast_to(maxima, dims)
    out_ref[1] = jnp.broadcast_to(totals, dims)
    out_ref[2] = jnp.dot(weights, rows_of(1), preferred_element_type=f32)


def join_blocks(heads, part_ref, tree_ref, lambdas_ref, gain_ref, out_ref):
    sources = part_ref.shape[0]
    head = lax.rem(lax.axis_index("kv"), heads)
    tile = (ROWS, LANES)
    pieces = jnp.concatenate(
        [part_ref[k][:, 2 * LANES :].astype(f32) for k in range(sources)], axis=0
    ).astype(bf16)
    pick_dims = (LANES, 4 * LANES)
    pick = jnp.where(row_iota(pick_dims) // 3 == lane_iota(pick_dims) // LANES, 1.0, 0.0)
    stats = jnp.dot(pieces, pick.astype(bf16), preferred_element_type=f32)
    attention = []
    for which in range(2):
        rows = slice(which * ROWS, (which + 1) * ROWS)
        low = 2 * which * LANES
        maxima = [stats[k * ROWS : (k + 1) * ROWS, low : low + LANES] for k in range(sources)]
        tree_max = tree_ref[0][rows]
        highest = tree_max
        for k in range(sources):
            highest = jnp.maximum(highest, maxima[k])
        scale = jnp.exp(tree_max - highest)
        totals = scale * tree_ref[1][rows]
        summed = scale * tree_ref[2][rows]
        for k in range(sources):
            factor = jnp.exp(maxima[k] - highest)
            total = stats[k * ROWS : (k + 1) * ROWS, low + LANES : low + 2 * LANES]
            totals = totals + factor * total
            block = part_ref[k][:, which * LANES : (which + 1) * LANES].astype(f32)
            summed = summed + factor * block
        attention.append(summed / totals)
    differ = attention[0] - lambdas_ref[head] * attention[1]
    mean = jnp.mean(differ * differ, axis=1, keepdims=True)
    normed = differ * lax.rsqrt(mean + epsilon)
    normed = (normed * gain_ref[...].astype(f32) * head_factor).astype(bf16)
    for owner in range(out_ref.shape[0]):
        out_ref[owner] = normed


def project_out(heads, head_out_ref, weight_ref, out_ref):
    groups = head_out_ref.shape[0] // heads
    total = None
    for head in range(heads):
        rows = jnp.concatenate(
            [head_out_ref[group * heads + head].astype(f32) for group in range(groups)], axis=0
        ).astype(bf16)
        weight = weight_ref[head * LANES : (head + 1) * LANES, :]
        term = jnp.dot(rows, weight, preferred_element_type=f32)
        total = term if total is None else total + term
    out_ref[...] = total.astype(bf16)


def add_groups(part_ref, out_ref):
    total = part_ref[0].astype(f32)
    for source in range(1, part_ref.shape[0]):
        total = total + part_ref[source].astype(f32)
    out_ref[...] = total.astype(bf16)


def exchange(pieces, axis):
    return lax.all_to_all(pieces, axis, split_axis=0, concat_axis=0, tiled=True)


def per_device(
    tokens,
    norm_gain,
    w_query1,
    w_query2,
    w_key1,
    w_key2,
    w_value,
    head_gain,
    lambdas,
    w_out,
    cache_keys,
    cache_values,
    lengths,
    accepted,
    parents,
):
    shards = lax.axis_size("kv")
    heads = cache_keys.shape[2]
    context = cache_keys.shape[1]
    seqs, nodes = parents.shape
    token_count = tokens.shape[0]
    qk_size = w_query1.shape[1] // heads
    width = tokens.shape[1] * shards
    assert token_count * heads == shards * ROWS and heads == 2 and nodes == 2 * ROWS
    assert 2 * qk_size == LANES and cache_values.shape[3] == LANES
    gain = norm_gain.reshape(1, -1)

    query_sent = call(
        functools.partial(query_parts, heads),
        shape((shards, 1, (ROWS + 1) * LANES), f32),
        [VMEM] * 4,
        "query_parts",
        2 * token_count * tokens.shape[1] * 2 * LANES,
    )(tokens, gain, w_query1, w_query2)
    query_got = exchange(query_sent, "kv")
    value_sent = call(
        functools.partial(value_parts, heads),
        shape((shards, ROWS, 2 * LANES), bf16),
        [VMEM] * 5,
        "value_parts",
        2 * token_count * tokens.shape[1] * 4 * LANES,
    )(tokens, gain, w_key1, w_key2, w_value)
    value_got = exchange(value_sent, "kv")
    keys_by_head = jnp.transpose(cache_keys, (2, 0, 1, 3))
    values_by_head = jnp.transpose(cache_values, (2, 0, 1, 3))

    query_mine, inverse = call(
        functools.partial(finish_queries, heads, width, qk_size ** (-0.5)),
        (shape((shards, ROWS, LANES), bf16), shape((ROWS, LANES), f32)),
        [VMEM],
        "finish_queries",
        1 << 20,
        out_specs=(VMEM, VMEM),
    )(query_got)
    queries = exchange(query_mine, "kv")
    fresh_mine = call(
        finish_values,
        shape((shards, ROWS, 2 * LANES), bf16),
        [VMEM, VMEM],
        "finish_values",
        1 << 20,
    )(value_got, inverse)
    fresh = exchange(fresh_mine, "kv")

    parts = call(
        functools.partial(attend_cache, heads),
        shape((shards, ROWS, 3 * LANES), bf16),
        [VMEM, VMEM, VMEM, SMEM, SMEM],
        "attend_cache",
        4 * token_count * 2 * heads * context * LANES,
    )(queries, keys_by_head, values_by_head, lengths, accepted)
    parts_got = exchange(parts, "kv")
    tree = call(
        functools.partial(attend_tree, heads),
        shape((3, 2 * ROWS, LANES), f32),
        [VMEM, VMEM, SMEM],
        "attend_tree",
        1 << 20,
        scratch=[pltpu.SMEM((nodes,), jnp.int32)],
    )(query_mine, fresh, parents)
    head_mine = call(
        functools.partial(join_blocks, heads),
        shape((shards, ROWS, LANES), bf16),
        [VMEM, VMEM, SMEM, VMEM],
        "join_blocks",
        1 << 22,
    )(parts_got, tree, lambdas, head_gain.reshape(1, -1))
    head_out = exchange(head_mine, "kv")
    product = call(
        functools.partial(project_out, heads),
        shape((token_count, w_out.shape[1]), bf16),
        [VMEM, VMEM],
        "project_out",
        2 * token_count * w_out.shape[0] * w_out.shape[1],
    )(head_out, w_out)
    groups = lax.axis_size("tp")
    product_got = exchange(product.reshape(groups, token_count // groups, -1), "tp")
    mixed = call(
        add_groups,
        shape((token_count // groups, w_out.shape[1]), bf16),
        [VMEM],
        "add_groups",
        1 << 20,
    )(product_got)

    by_kind = fresh.reshape(token_count // ROWS, 2, ROWS, heads, LANES)
    by_kind = jnp.moveaxis(by_kind, 1, 0).reshape(2, seqs, nodes, heads, LANES)
    valid_len = lengths + accepted
    positions = lax.axis_index("kv") * context + jnp.arange(context, dtype=jnp.int32)
    offsets = positions[None, :] - valid_len[:, None]
    picker = (offsets[:, :, None] == jnp.arange(nodes, dtype=jnp.int32)).astype(bf16)
    landed = ((offsets >= 0) & (offsets < nodes))[:, :, None, None]

    def write(cache, rows):
        placed = jnp.einsum("scp,sphd->schd", picker, rows, preferred_element_type=f32)
        return jnp.where(landed, placed.astype(bf16), cache)

    return mixed, write(cache_keys, by_kind[0]), write(cache_values, by_kind[1])


def solution(mesh):
    return jax.shard_map(
        per_device,
        mesh=mesh,
        in_specs=(
            P("grp", "kv"),
            P("kv"),
            P("kv", "tp"),
            P("kv", "tp"),
            P("kv", "tp"),
            P("kv", "tp"),
            P("kv", "tp"),
            P(),
            P("tp"),
            P("tp", "kv"),
            P("grp", "kv", "tp", None),
            P("grp", "kv", "tp", None),
            P("grp"),
            P("grp"),
            P("grp", None),
        ),
        out_specs=(P(("grp", "tp"), "kv"), P("grp", "kv", "tp", None), P("grp", "kv", "tp", None)),
        check_vma=False,
    )
```

```python
import functools

import jax
import jax.numpy as jnp
from jax import lax
from jax.experimental import pallas as pl
from jax.experimental.pallas import tpu as pltpu
from jax.sharding import PartitionSpec as P

epsilon = 1e-06
masked_fill = -1e30
head_factor = 0.8
LANES = 128
ROWS = 8
HALF = ROWS // 2
PIECES = 6
VMEM_BYTES = 16 << 20

f32 = jnp.float32
bf16 = jnp.bfloat16
VMEM = pl.BlockSpec(memory_space=pltpu.VMEM)
SMEM = pl.BlockSpec(memory_space=pltpu.SMEM)


def call(body, out_shape, in_specs, name, flops, out_specs=VMEM, scratch=()):
    return pl.pallas_call(
        body,
        out_shape=out_shape,
        in_specs=in_specs,
        out_specs=out_specs,
        scratch_shapes=scratch,
        compiler_params=pltpu.CompilerParams(vmem_limit_bytes=VMEM_BYTES),
        cost_estimate=pl.CostEstimate(flops=flops, bytes_accessed=1 << 16, transcendentals=0),
        name=name,
    )


def shape(dims, dtype):
    return jax.ShapeDtypeStruct(dims, dtype)


def lane_iota(dims):
    return lax.broadcasted_iota(jnp.int32, dims, len(dims) - 1)


def row_iota(dims):
    return lax.broadcasted_iota(jnp.int32, dims, len(dims) - 2)


def scale_tokens(tokens_ref, gain_ref):
    wide = tokens_ref[...].astype(f32)
    return wide, (wide * gain_ref[...].astype(f32)).astype(bf16)


def by_head(first, second, head):
    half = LANES // 2
    left = first[:, head * half : (head + 1) * half]
    right = second[:, head * half : (head + 1) * half]
    return jnp.concatenate([left, right], axis=1)


def in_pieces(value):
    high = value.astype(bf16).astype(f32)
    rest = value - high
    middle = rest.astype(bf16).astype(f32)
    return (high, middle, rest - middle)


def put_halves(out_ref, owner, at, tile):
    for half in range(2):
        lanes = slice((at + half) * LANES, (at + half + 1) * LANES)
        out_ref[owner, :, lanes] = tile[half * HALF : (half + 1) * HALF].astype(bf16)


def take_halves(value, at):
    low, high = at * LANES, (at + 1) * LANES
    return jnp.concatenate([value[:, low:high], value[:, high : high + LANES]], axis=0)


def projection_parts(
    heads, tokens_ref, gain_ref, q1_ref, q2_ref, k1_ref, k2_ref, v_ref, out_ref
):
    wide, scaled = scale_tokens(tokens_ref, gain_ref)
    first, second, key1, key2, value = [
        jnp.dot(scaled, ref[...], preferred_element_type=f32)
        for ref in (q1_ref, q2_ref, k1_ref, k2_ref, v_ref)
    ]
    dims = wide.shape
    squares = in_pieces(jnp.sum(wide * wide, axis=1, keepdims=True))
    at = lane_iota(dims) - jnp.where(lax.rem(row_iota(dims), ROWS) >= HALF, 3, 0)
    stats = jnp.zeros(dims, f32)
    for k, piece in enumerate(squares):
        stats = jnp.where(at == k, piece, stats)
    queries = [by_head(first, second, head) for head in range(heads)]
    highs = [query.astype(bf16).astype(f32) for query in queries]
    lows = [query - high for query, high in zip(queries, highs)]
    keys = [by_head(key1, key2, head) for head in range(heads)]
    values = [value[:, head * LANES : (head + 1) * LANES] for head in range(heads)]
    for group in range(dims[0] // ROWS):
        rows = slice(group * ROWS, (group + 1) * ROWS)
        tile = stats[rows]
        packed = tile[:HALF] + tile[HALF:]
        for head in range(heads):
            owner = group * heads + head
            put_halves(out_ref, owner, 0, highs[head][rows])
            put_halves(out_ref, owner, 2, lows[head][rows])
            for column, array in enumerate((keys, values)[head]):
                put_halves(out_ref, owner, 4 + 2 * column, array[rows])
            out_ref[owner, :, 8 * LANES :] = packed.astype(bf16)


def finish_projections(width, factor, part_ref, out_ref):
    total = part_ref[0].astype(f32)
    for source in range(1, part_ref.shape[0]):
        total = total + part_ref[source].astype(f32)
    stats = total[:, 8 * LANES :]
    lane = lane_iota(stats.shape)
    squares = jnp.concatenate(
        [
            jnp.sum(jnp.where(lane // 3 == half, stats, 0.0), axis=1, keepdims=True)
            for half in range(2)
        ],
        axis=0,
    )
    inverse = lax.rsqrt(squares / width + epsilon)
    query = (take_halves(total, 0) + take_halves(total, 2)) * inverse * factor
    fresh = [take_halves(total, at) * inverse for at in (4, 6)]
    mine = jnp.concatenate([query] + fresh, axis=1).astype(bf16)
    for owner in range(out_ref.shape[0]):
        out_ref[owner] = mine


def two_maps(query):
    low = lane_iota(query.shape) < LANES // 2
    zero = jnp.zeros_like(query)
    return jnp.concatenate(
        [jnp.where(low, query, zero), jnp.where(low, zero, query)], axis=0
    ).astype(bf16)


def softmax_block(scores, visible):
    scores = jnp.where(visible, scores, masked_fill)
    maxima = jnp.max(scores, axis=1, keepdims=True)
    weights = jnp.where(visible, jnp.exp(scores - maxima), 0.0)
    return maxima, jnp.sum(weights, axis=1, keepdims=True), weights.astype(bf16)


def contract_last(left, right):
    return lax.dot_general(left, right, (((1,), (1,)), ((), ())), preferred_element_type=f32)


def attend_cache(heads, query_ref, keys_ref, values_ref, lengths_ref, accepted_ref, out_ref):
    seqs, context = keys_ref.shape[1], keys_ref.shape[2]
    start = lax.axis_index("kv") * context
    for seq in range(seqs):
        limit = lengths_ref[seq] + accepted_ref[seq] - start
        for head in range(heads):
            owners = [(2 * seq + half) * heads + head for half in range(2)]
            query = jnp.concatenate([query_ref[o][:, :LANES].astype(f32) for o in owners], axis=0)
            both = two_maps(query)
            scores = contract_last(both, keys_ref[head, seq])
            visible = lane_iota(scores.shape) < limit
            maxima, totals, weights = softmax_block(scores, visible)
            summed = jnp.dot(weights, values_ref[head, seq], preferred_element_type=f32)
            dims = summed.shape
            count = dims[0] // 2
            row = row_iota(dims)
            at = lane_iota(dims) - jnp.where(row >= count, PIECES, 0)
            at = at - jnp.where(lax.rem(row, ROWS) >= HALF, 2 * PIECES, 0)
            stats = jnp.zeros(dims, f32)
            for k, piece in enumerate(in_pieces(maxima) + in_pieces(totals)):
                stats = jnp.where(at == k, piece, stats)
            for half, owner in enumerate(owners):
                low, high = half * ROWS, count + half * ROWS
                first, second = slice(low, low + ROWS), slice(high, high + ROWS)
                put_halves(out_ref, owner, 0, summed[first])
                put_halves(out_ref, owner, 2, summed[second])
                tile = stats[first] + stats[second]
                out_ref[owner, :, 4 * LANES :] = (tile[:HALF] + tile[HALF:]).astype(bf16)


def attend_tree(heads, mine_ref, fresh_ref, parents_ref, out_ref, seen_ref):
    me = lax.axis_index("kv")
    head, group = lax.rem(me, heads), me // heads
    seq, half = group // 2, lax.rem(group, 2)
    nodes = parents_ref.shape[1]
    for node in range(nodes):
        parent = parents_ref[seq, node]
        above = jnp.where(parent >= 0, seen_ref[jnp.maximum(parent, 0)], 0) if node else 0
        seen_ref[node] = above | (1 << node)

    def rows_of(kind):
        tiles = []
        for part in range(2):
            both = fresh_ref[(2 * seq + part) * heads + kind].astype(f32)
            tiles.append(
                jnp.where(head == 0, both[:, LANES : 2 * LANES], both[:, 2 * LANES :])
            )
        tiles.append(jnp.zeros((LANES - nodes, LANES), f32))
        return jnp.concatenate(tiles, axis=0).astype(bf16)

    both = two_maps(mine_ref[0][:, :LANES].astype(f32))
    scores = contract_last(both, rows_of(0))
    dims = scores.shape
    row = lax.rem(row_iota(dims), ROWS)
    bits = jnp.zeros(dims, jnp.int32)
    for k in range(ROWS):
        bits = jnp.where(row == k, seen_ref[half * ROWS + k], bits)
    lane = lane_iota(dims)
    visible = (lane < nodes) & ((lax.shift_right_logical(bits, jnp.minimum(lane, 31)) & 1) == 1)
    maxima, totals, weights = softmax_block(scores, visible)
    out_ref[0] = jnp.broadcast_to(maxima, dims)
    out_ref[1] = jnp.broadcast_to(totals, dims)
    out_ref[2] = jnp.dot(weights, rows_of(1), preferred_element_type=f32)


def join_blocks(heads, part_ref, tree_ref, lambdas_ref, gain_ref, out_ref):
    sources = part_ref.shape[0]
    head = lax.rem(lax.axis_index("kv"), heads)
    tile = (ROWS, LANES)
    pieces = []
    for k in range(sources):
        packed = part_ref[k][:, 4 * LANES :].astype(f32)
        pieces += [packed, pltpu.roll(packed, LANES - 2 * PIECES, 1)]
    pieces = jnp.concatenate(pieces, axis=0).astype(bf16)
    pick_dims = (LANES, 4 * LANES)
    pick = jnp.where(row_iota(pick_dims) // 3 == lane_iota(pick_dims) // LANES, 1.0, 0.0)
    stats = jnp.dot(pieces, pick.astype(bf16), preferred_element_type=f32)
    attention = []
    for which in range(2):
        rows = slice(which * ROWS, (which + 1) * ROWS)
        low = 2 * which * LANES
        maxima = [stats[k * ROWS : (k + 1) * ROWS, low : low + LANES] for k in range(sources)]
        tree_max = tree_ref[0][rows]
        highest = tree_max
        for k in range(sources):
            highest = jnp.maximum(highest, maxima[k])
        scale = jnp.exp(tree_max - highest)
        totals = scale * tree_ref[1][rows]
        summed = scale * tree_ref[2][rows]
        for k in range(sources):
            factor = jnp.exp(maxima[k] - highest)
            total = stats[k * ROWS : (k + 1) * ROWS, low + LANES : low + 2 * LANES]
            totals = totals + factor * total
            block = part_ref[k][:, 2 * which * LANES : 2 * (which + 1) * LANES].astype(f32)
            summed = summed + factor * take_halves(block, 0)
        attention.append(summed / totals)
    differ = attention[0] - lambdas_ref[head] * attention[1]
    mean = jnp.mean(differ * differ, axis=1, keepdims=True)
    normed = differ * lax.rsqrt(mean + epsilon)
    normed = (normed * gain_ref[...].astype(f32) * head_factor).astype(bf16)
    for owner in range(out_ref.shape[0]):
        out_ref[owner] = normed


def project_out(heads, head_out_ref, weight_ref, out_ref):
    groups = head_out_ref.shape[0] // heads
    total = None
    for head in range(heads):
        rows = jnp.concatenate(
            [head_out_ref[group * heads + head].astype(f32) for group in range(groups)], axis=0
        ).astype(bf16)
        weight = weight_ref[head * LANES : (head + 1) * LANES, :]
        term = jnp.dot(rows, weight, preferred_element_type=f32)
        total = term if total is None else total + term
    out_ref[...] = total.astype(bf16)


def add_groups(part_ref, out_ref):
    total = part_ref[0].astype(f32)
    for source in range(1, part_ref.shape[0]):
        total = total + part_ref[source].astype(f32)
    out_ref[...] = total.astype(bf16)


def exchange(pieces, axis):
    return lax.all_to_all(pieces, axis, split_axis=0, concat_axis=0, tiled=True)


def per_device(
    tokens,
    norm_gain,
    w_query1,
    w_query2,
    w_key1,
    w_key2,
    w_value,
    head_gain,
    lambdas,
    w_out,
    cache_keys,
    cache_values,
    lengths,
    accepted,
    parents,
):
    shards = lax.axis_size("kv")
    heads = cache_keys.shape[2]
    context = cache_keys.shape[1]
    seqs, nodes = parents.shape
    token_count = tokens.shape[0]
    qk_size = w_query1.shape[1] // heads
    width = tokens.shape[1] * shards
    assert token_count * heads == shards * ROWS and heads == 2 and nodes == 2 * ROWS
    assert 2 * qk_size == LANES and cache_values.shape[3] == LANES
    gain = norm_gain.reshape(1, -1)

    sent = call(
        functools.partial(projection_parts, heads),
        shape((shards, HALF, 9 * LANES), bf16),
        [VMEM] * 7,
        "projection_parts",
        2 * token_count * tokens.shape[1] * 6 * LANES,
    )(tokens, gain, w_query1, w_query2, w_key1, w_key2, w_value)
    got = exchange(sent, "kv")
    keys_by_head = jnp.transpose(cache_keys, (2, 0, 1, 3))
    values_by_head = jnp.transpose(cache_values, (2, 0, 1, 3))
    mine = call(
        functools.partial(finish_projections, width, qk_size ** (-0.5)),
        shape((shards, ROWS, 3 * LANES), bf16),
        [VMEM],
        "finish_projections",
        1 << 20,
    )(got)
    projected = exchange(mine, "kv")

    parts = call(
        functools.partial(attend_cache, heads),
        shape((shards, HALF, 5 * LANES), bf16),
        [VMEM, VMEM, VMEM, SMEM, SMEM],
        "attend_cache",
        4 * token_count * 2 * heads * context * LANES,
    )(projected, keys_by_head, values_by_head, lengths, accepted)
    parts_got = exchange(parts, "kv")
    tree = call(
        functools.partial(attend_tree, heads),
        shape((3, 2 * ROWS, LANES), f32),
        [VMEM, VMEM, SMEM],
        "attend_tree",
        1 << 20,
        scratch=[pltpu.SMEM((nodes,), jnp.int32)],
    )(mine, projected, parents)
    head_mine = call(
        functools.partial(join_blocks, heads),
        shape((shards, ROWS, LANES), bf16),
        [VMEM, VMEM, SMEM, VMEM],
        "join_blocks",
        1 << 22,
    )(parts_got, tree, lambdas, head_gain.reshape(1, -1))
    head_out = exchange(head_mine, "kv")
    product = call(
        functools.partial(project_out, heads),
        shape((token_count, w_out.shape[1]), bf16),
        [VMEM, VMEM],
        "project_out",
        2 * token_count * w_out.shape[0] * w_out.shape[1],
    )(head_out, w_out)
    groups = lax.axis_size("tp")
    product_got = exchange(product.reshape(groups, token_count // groups, -1), "tp")
    mixed = call(
        add_groups,
        shape((token_count // groups, w_out.shape[1]), bf16),
        [VMEM],
        "add_groups",
        1 << 20,
    )(product_got)

    by_kind = projected[:, :, LANES:].reshape(token_count // ROWS, 2, ROWS, heads, LANES)
    by_kind = jnp.moveaxis(by_kind, 1, 0).reshape(2, seqs, nodes, heads, LANES)
    valid_len = lengths + accepted
    positions = lax.axis_index("kv") * context + jnp.arange(context, dtype=jnp.int32)
    offsets = positions[None, :] - valid_len[:, None]
    picker = (offsets[:, :, None] == jnp.arange(nodes, dtype=jnp.int32)).astype(bf16)
    landed = ((offsets >= 0) & (offsets < nodes))[:, :, None, None]

    def write(cache, rows):
        placed = jnp.einsum("scp,sphd->schd", picker, rows, preferred_element_type=f32)
        return jnp.where(landed, placed.astype(bf16), cache)

    return mixed, write(cache_keys, by_kind[0]), write(cache_values, by_kind[1])


def solution(mesh):
    return jax.shard_map(
        per_device,
        mesh=mesh,
        in_specs=(
            P("grp", "kv"),
            P("kv"),
            P("kv", "tp"),
            P("kv", "tp"),
            P("kv", "tp"),
            P("kv", "tp"),
            P("kv", "tp"),
            P(),
            P("tp"),
            P("tp", "kv"),
            P("grp", "kv", "tp", None),
            P("grp", "kv", "tp", None),
            P("grp"),
            P("grp"),
            P("grp", None),
        ),
        out_specs=(P(("grp", "tp"), "kv"), P("grp", "kv", "tp", None), P("grp", "kv", "tp", None)),
        check_vma=False,
    )
```
